32 devices in a mesh: ep: 8 (over z, y), tp: 4 (over x, core).
Axes of the slice: x: 2, y: 2, z: 4, core: 2. Of those that a mesh axis runs over, the one named last changes fastest.
Arguments:
- queries: bfloat16 [4096, 1024], P('ep', 'tp'), may hold values from -8 to 8
- key_rows: bfloat16 [4096, 1024], P('ep', 'tp'), may hold values from -8 to 8
- value_rows: bfloat16 [4096, 1024], P('ep', 'tp'), may hold values from -6 to 6
- lambdas: float32 [8], P('tp'), may hold values from 0.3 to 0.8
- head_gain: float32 [128], replicated, may hold values from 0.1 to 1.9
- out_weight: bfloat16 [1024, 2048], P('tp'), may hold values from -0.1875 to 0.1875
- moe_input: bfloat16 [4096, 2048], P(('ep', 'tp')), may hold values from -400 to 400
- moe_gain: float32 [2048], replicated, may hold values from 0.1 to 1.9
- routes: int32 [4096, 2], P(('ep', 'tp')), may hold values from 0 to 7, all different within a row; in each aligned block of 128 rows (0 to 127, 128 to 255, ...) at most 40 rows name the same one
- route_logits: float32 [4096, 2], P(('ep', 'tp')), may hold values from -6 to 6
- expert_gate: bfloat16 [8, 2048, 3584], P('ep', None, 'tp'), may hold values from -0.125 to 0.125
- expert_up: bfloat16 [8, 2048, 3584], P('ep', None, 'tp'), may hold values from -0.125 to 0.125
- expert_down: bfloat16 [8, 3584, 2048], P('ep', 'tp'), may hold values from -0.09375 to 0.09375
Outputs:
- mixer_out: bfloat16 [4096, 2048], P(('ep', 'tp'))
- expert_out: bfloat16 [4096, 2048], P(('ep', 'tp'))
The draws below stay inside these ranges and needn't reach their ends.
Inputs may be any that keep to these rules, and one draw needn't show every extreme that they name: `routes`: each token names 2 different experts. Among the tokens of one device no expert is named more than 40 times, and in every draw some expert is named exactly 40 times by the tokens of some device.
All inputs are finite; a program needn't handle non-finite values.
Results may differ from the reference program's by a relative error of at most 0.014.
Values may be sent and summed in bfloat16 or wider, within the bound.
No kernel may reach another device: no remote copies, remote signals or barrier semaphores. Data moves between devices by JAX's collectives and lax.ppermute only.
A program may use at most 128 MiB of HBM per device.

```python
import math
import jax
import jax.numpy as jnp
import numpy as np
from jax import lax

D = 2048
HEADS = 8
HEAD = 64
VDIM = 128
FFE = 3584
TOP = 2
TOK2_DEV = 128
SEQ = 4096
TOKENS2 = 4096
EXPERTS = 8
CAP = 40
N_EP = 8
N_TP = 4


def drawn_pairs(key):
    folded = jax.random.fold_in(key, 17)
    key_query, key_keys = jax.random.split(folded, 2)
    row_width = HEADS * 2 * HEAD
    spread = 1.32
    query_draw = jax.random.normal(key_query, (SEQ, row_width), jnp.float32) * spread
    key_draw = jax.random.normal(key_keys, (SEQ, row_width), jnp.float32) * spread
    return (jnp.clip(query_draw, -8.0, 8.0), jnp.clip(key_draw, -8.0, 8.0))


def draw_queries(key, part):
    return drawn_pairs(key)[0].astype(jnp.bfloat16)


def draw_key_rows(key, part):
    return drawn_pairs(key)[1].astype(jnp.bfloat16)


def draw_moe_input(key, part):
    folded = jax.random.fold_in(key, 23)
    key_rows_scale, key_cols_scale, key_sample = jax.random.split(folded, 3)
    row_scale = jnp.exp(jax.random.uniform(key_rows_scale, (TOKENS2, 1), jnp.float32, 0.0, math.log(10.0)))
    column_scale = jnp.exp(jax.random.uniform(key_cols_scale, (1, D), jnp.float32, 0.0, math.log(10.0)))
    sample = jax.random.normal(key_sample, (TOKENS2, D), jnp.float32)
    return jnp.clip(sample * row_scale * column_scale, -400.0, 400.0).astype(jnp.bfloat16)


def shard_levels(key, shape, cuts, least, top_value):
    factor_of, own = 1.0, jax.random.fold_in(key, 6)
    for dim, shards_of in cuts:
        draws = jnp.exp(jax.random.uniform(jax.random.fold_in(own, dim), (shards_of,), jnp.float32, least / len(cuts), top_value / len(cuts)))
        factor_of = factor_of * jnp.repeat(draws, shape[dim] // shards_of).reshape([-1 if axis == dim else 1 for axis in range(len(shape))])
    return factor_of


def assign_block(rng, own, number, rows, count, top, most, slope):
    order = jax.random.permutation(rng, count)
    crowded, usual = shares(count, rows * top, most, slope, True), shares(count, rows * top, most, slope, False)
    places = jnp.arange(count)

    def named(lengths, rotation):
        used = int((lengths > 0).sum())
        fixed = max(1, used // 4)
        shifted = fixed + (places - fixed + rotation * (used - fixed)) % max(1, count - fixed)
        return jnp.zeros((count,), jnp.int32).at[order[jnp.where(places < fixed, places, shifted)]].set(jnp.asarray(lengths, jnp.int32))

    lengths = jnp.where(number % 4 == 0, named(crowded, number // 4), named(usual, number - number // 4 - 1))
    mixed = jax.random.permutation(jax.random.fold_in(own, 3), count)
    donor, taker = mixed[0:count // 2 * 2:2], mixed[1:count // 2 * 2:2]
    room = jnp.minimum(lengths[donor] - 1, most - lengths[taker]) // 2
    room = jnp.where((donor == order[0]) | (taker == order[0]) | (lengths[taker] == 0), 0, jnp.maximum(room, 0))
    shifted = jax.random.randint(jax.random.fold_in(own, 4), (count // 2,), 0, 1 << 20) % (room + 1)
    lengths = lengths.at[donor].add(-shifted).at[taker].add(shifted)
    items = jnp.searchsorted(jnp.cumsum(lengths), jnp.arange(rows * top), side="right").astype(jnp.int32)
    table = items.reshape(top, rows).T
    table = table[jax.random.permutation(jax.random.fold_in(own, 1), rows)]
    rotation = jax.random.randint(jax.random.fold_in(own, 2), (rows, 1), 0, top)
    return jnp.take_along_axis(table, (jnp.arange(top)[None, :] + rotation) % top, axis=1)


def shares(number_of, total, most, slope, full):
    loads = [(1 << 20) // math.isqrt(rank ** slope) + 1 for rank in range(1, number_of + 1)]
    largest = most if full else min(most, max(-(-total // number_of), total * loads[0] // sum(loads)))
    least = 1 if total - largest >= number_of - 1 else 0
    counts, rest = [largest] + [least] * (number_of - 1), total - largest - least * (number_of - 1)
    while rest > 0:
        candidates = [i for i in range(1, number_of) if counts[i] < largest] or [i for i in range(1, number_of) if counts[i] < most]
        whole, left = sum([loads[i] for i in candidates]), rest
        for i in candidates:
            more = min(most - counts[i], max(1, left * loads[i] // whole), rest)
            counts[i] = counts[i] + more
            rest = rest - more
    return np.array(counts)


def normal_values(key, dims, deviation, most, cuts=(), kind=jnp.bfloat16):
    values = deviation * jax.random.normal(key, dims, jnp.float32)
    if cuts:
        values = values * shard_levels(key, dims, cuts, -0.22, 0.18)
    return jnp.clip(values, -most, most).astype(kind)


def setup_inputs(seed: int = 0) -> dict:
    seeds = jax.random.split(jax.random.key(seed), 14)
    queries = draw_queries(jax.random.fold_in(seeds[13], 71), 0)
    key_rows = draw_key_rows(jax.random.fold_in(seeds[13], 71), 0)
    value_rows = normal_values(seeds[2], (SEQ, HEADS * VDIM), 1.0, 6.0, ((0, 8), (1, 4)))
    lambdas = jnp.clip(0.3 + 0.5 * jax.random.uniform(seeds[3], (HEADS,), jnp.float32) ** shard_levels(seeds[3], (HEADS,), ((0, 4),), -0.2, 0.2), 0.3, 0.8)
    head_gain = jnp.clip(1.0 + 0.18 * jax.random.normal(seeds[4], (VDIM,), jnp.float32), 0.1, 1.9)
    out_weight = normal_values(seeds[5], (HEADS * VDIM, D), (HEADS * VDIM) ** -0.5, 0.1875, ((0, 4),))
    moe_input = draw_moe_input(jax.random.fold_in(seeds[13], 71), 0)
    moe_gain = jnp.clip(1.0 + 0.18 * jax.random.normal(seeds[7], (D,), jnp.float32), 0.1, 1.9)
    routes_keys = jax.random.split(jax.random.fold_in(seeds[8], 1), TOKENS2 // TOK2_DEV)
    routes_turns = jax.random.permutation(jax.random.fold_in(seeds[8], 3), TOKENS2 // TOK2_DEV)
    routes = jax.vmap(lambda own, number: assign_block(jax.random.fold_in(seeds[8], 2), own, number, TOK2_DEV, EXPERTS, TOP, CAP, 1))(routes_keys, routes_turns).reshape((TOKENS2, TOP))
    route_logits = normal_values(seeds[9], (TOKENS2, TOP), 1.5, 6.0, ((0, 32),), jnp.float32)
    expert_gate = normal_values(seeds[10], (EXPERTS, D, FFE), D ** -0.5, 0.125, ((0, 8), (2, 4)))
    expert_up = normal_values(seeds[11], (EXPERTS, D, FFE), D ** -0.5, 0.125, ((0, 8), (2, 4)))
    expert_down = normal_values(seeds[12], (EXPERTS, FFE, D), FFE ** -0.5, 0.09375, ((0, 8), (1, 4)))
    return dict(queries=queries, key_rows=key_rows, value_rows=value_rows, lambdas=lambdas, head_gain=head_gain, out_weight=out_weight, moe_input=moe_input, moe_gain=moe_gain, routes=routes, route_logits=route_logits, expert_gate=expert_gate, expert_up=expert_up, expert_down=expert_down)


epsilon = 1e-06
init_lambda = 0.2

def one_head(query_head, key_head, value_head, lambda_head, head_gain):
    seq_len = query_head.shape[0]
    block_rows = math.gcd(seq_len, 512)
    score_scale = HEAD ** (-0.5)
    blocks = query_head.reshape(seq_len // block_rows, block_rows, 2, HEAD)

    def one_block(query_block):
        outputs = []
        for map_index in range(2):
            scores = jnp.dot(query_block[:, map_index], key_head[:, map_index].T, preferred_element_type=jnp.float32) * score_scale
            maxima = lax.optimization_barrier(jnp.max(scores, axis=-1, keepdims=True))
            exponent = jnp.exp(scores - maxima)
            totals = lax.optimization_barrier(jnp.sum(exponent, axis=-1, keepdims=True))
            product = jnp.dot(exponent.astype(jnp.bfloat16), value_head, preferred_element_type=jnp.float32)
            outputs.append(product / totals)
        head_out = outputs[0] - lambda_head * outputs[1]
        mean_square = lax.optimization_barrier(jnp.mean(head_out * head_out, axis=-1, keepdims=True))
        return (head_out * lax.rsqrt(mean_square + epsilon) * head_gain * (1.0 - init_lambda)).astype(jnp.bfloat16)
    return lax.map(one_block, blocks).reshape(seq_len, VDIM)

def reference(queries, key_rows, value_rows, lambdas, head_gain, out_weight, moe_input, moe_gain, routes, route_logits, expert_gate, expert_up, expert_down):
    seq_len = queries.shape[0]
    query_heads = queries.reshape(seq_len, HEADS, 2, HEAD).transpose(1, 0, 2, 3)
    key_heads = key_rows.reshape(seq_len, HEADS, 2, HEAD).transpose(1, 0, 2, 3)
    value_heads = value_rows.reshape(seq_len, HEADS, VDIM).transpose(1, 0, 2)

    def head_step(packed):
        return one_head(packed[0], packed[1], packed[2], packed[3], head_gain)
    attended = lax.map(head_step, (query_heads, key_heads, value_heads, lambdas))
    group_heads = HEADS // N_TP
    weight_heads = out_weight.reshape(HEADS, VDIM, D)
    mixer_total = jnp.zeros((seq_len, D), jnp.float32)
    for group_index in range(N_TP):
        lower = group_index * group_heads
        partial_value = jnp.einsum('hqe,hed->qd', attended[lower:lower + group_heads].astype(jnp.float32), weight_heads[lower:lower + group_heads].astype(jnp.float32))
        mixer_total = mixer_total + lax.optimization_barrier(partial_value.astype(jnp.bfloat16)).astype(jnp.float32)
    mixer_out = mixer_total.astype(jnp.bfloat16)
    moe_float = moe_input.astype(jnp.float32)
    normed = (moe_float * lax.rsqrt(lax.optimization_barrier(jnp.mean(moe_float * moe_float, axis=-1, keepdims=True)) + epsilon) * moe_gain).astype(jnp.bfloat16)
    gate_weights = jax.nn.softmax(route_logits, axis=-1)
    device_count = N_EP * N_TP
    per_device = TOK2_DEV * TOP
    flat_routes = routes.reshape(device_count, per_device)
    chosen = (flat_routes[:, :, None] == jnp.arange(EXPERTS, dtype=jnp.int32)[None, None, :]).astype(jnp.int32)
    slot_rank = lax.optimization_barrier(jnp.sum((jnp.cumsum(chosen, axis=1) - chosen) * chosen, axis=2))
    device_ids = jnp.arange(device_count, dtype=jnp.int32)[:, None] * jnp.ones((1, per_device), jnp.int32)
    positions = (device_ids * CAP + slot_rank).reshape(-1).astype(jnp.int32)
    row_ids = (jnp.arange(device_count * per_device, dtype=jnp.int32) // TOP).astype(jnp.int32)
    expert_ids = flat_routes.reshape(-1).astype(jnp.int32)
    slot_table = jnp.full((EXPERTS, device_count * CAP), TOKENS2, jnp.int32).at[expert_ids, positions].set(row_ids)
    padded = jnp.concatenate([normed, jnp.zeros((1, D), jnp.bfloat16)], axis=0)
    width_part = FFE // N_TP

    def one_expert(packed):
        indices, gate_matrix, up_matrix, down_matrix = packed
        rows_in = padded[indices]
        gate_part = jnp.dot(rows_in, gate_matrix, preferred_element_type=jnp.float32)
        up_part = jnp.dot(rows_in, up_matrix, preferred_element_type=jnp.float32)
        hidden = (jax.nn.silu(gate_part) * up_part).astype(jnp.bfloat16)
        summed = jnp.zeros((rows_in.shape[0], D), jnp.float32)
        for group_index in range(N_TP):
            lower = group_index * width_part
            partial_value = jnp.dot(hidden[:, lower:lower + width_part], down_matrix[lower:lower + width_part], preferred_element_type=jnp.float32)
            summed = summed + lax.optimization_barrier(partial_value.astype(jnp.bfloat16)).astype(jnp.float32)
        return summed.astype(jnp.bfloat16)
    replies = lax.map(one_expert, (slot_table, expert_gate, expert_up, expert_down))
    picked = replies[expert_ids, positions].reshape(TOKENS2, TOP, D)
    expert_out = lax.optimization_barrier(jnp.sum(gate_weights[:, :, None] * picked.astype(jnp.float32), axis=1)).astype(jnp.bfloat16)
    return (mixer_out, expert_out)
```

```python
import functools

import jax
import jax.numpy as jnp
from jax import lax
from jax.experimental import pallas as pl
from jax.experimental.pallas import tpu as pltpu
from jax.sharding import PartitionSpec as P

epsilon = 1e-06
init_lambda = 0.2
vmem_bytes = 60 * 1024 * 1024


whole_vmem = pl.BlockSpec(memory_space=pltpu.VMEM)


def capacity(tokens, top_count, experts):
    return max(2, (top_count * tokens * 5 + 4 * experts - 1) // (4 * experts))


def swap(array, axis, mask):
    size = lax.axis_size(axis)
    return lax.ppermute(array, axis, [(i, i ^ mask) for i in range(size)])


def dispatch_kernel(cap, x_ref, gain_ref, hops_ref, ranks_ref, *blocks):
    tokens, width = x_ref.shape
    rows = x_ref[...].astype(jnp.float32)
    mean_square = jnp.mean(rows * rows, axis=-1, keepdims=True)
    normed = (rows * lax.rsqrt(mean_square + epsilon) * gain_ref[...]).astype(jnp.bfloat16)
    count = len(blocks)
    top = hops_ref.shape[0]
    earlier = lax.broadcasted_iota(jnp.int32, (tokens, tokens), 0)
    later = lax.broadcasted_iota(jnp.int32, (tokens, tokens), 1)
    before = (earlier < later).astype(jnp.float32).astype(jnp.bfloat16)
    hop_ids = lax.broadcasted_iota(jnp.int32, (count, tokens), 0)
    base = jnp.zeros((count, 1), jnp.float32)
    ranks = []
    for j in range(top):
        chosen = (hops_ref[j : j + 1, :] == hop_ids).astype(jnp.float32)
        prefix = jnp.dot(chosen.astype(jnp.bfloat16), before, preferred_element_type=jnp.float32)
        rank = jnp.sum(chosen * (prefix + base), axis=0, keepdims=True)
        base = base + jnp.sum(chosen, axis=1, keepdims=True)
        ranks.append(rank.astype(jnp.int32))
        ranks_ref[j : j + 1, :] = ranks[-1]
    places = lax.broadcasted_iota(jnp.int32, (cap, tokens), 0)
    for k, block in enumerate(blocks):
        picked = jnp.zeros((cap, tokens), jnp.float32)
        for j in range(top):
            hit = (hops_ref[j : j + 1, :] == k) & (ranks[j] == places)
            picked = picked + hit.astype(jnp.float32)
        block[...] = jnp.dot(
            picked.astype(jnp.bfloat16), normed, preferred_element_type=jnp.float32
        ).astype(jnp.bfloat16)


def dispatch(moe_input, moe_gain, hops, cap, count):
    tokens, width = moe_input.shape
    shapes = [jax.ShapeDtypeStruct(hops.shape, jnp.int32)]
    shapes += [jax.ShapeDtypeStruct((cap, width), jnp.bfloat16)] * count
    out = pl.pallas_call(
        functools.partial(dispatch_kernel, cap),
        out_shape=shapes,
        in_specs=[whole_vmem] * 3,
        out_specs=[whole_vmem] * len(shapes),
        cost_estimate=pl.CostEstimate(flops=2 * cap * count * tokens * width, bytes_accessed=4 * tokens * width, transcendentals=0),
        name="dispatch",
    )(moe_input, moe_gain.reshape(1, -1), hops)
    return out[0], list(out[1:])


def combine_kernel(hops_ref, ranks_ref, logits_ref, *refs):
    blocks, out_ref = refs[:-1], refs[-1]
    top, tokens = hops_ref.shape
    cap = blocks[0].shape[0]
    logits = logits_ref[...]
    peak = jnp.max(logits, axis=0, keepdims=True)
    raised = jnp.exp(logits - peak)
    gates = raised / jnp.sum(raised, axis=0, keepdims=True)
    places = lax.broadcasted_iota(jnp.int32, (cap, tokens), 0)
    total = jnp.zeros(out_ref.shape, jnp.float32)
    for k, block in enumerate(blocks):
        weight = jnp.zeros((cap, tokens), jnp.float32)
        for j in range(top):
            hit = (hops_ref[j : j + 1, :] == k) & (ranks_ref[j : j + 1, :] == places)
            weight = weight + jnp.where(hit, gates[j : j + 1, :], 0.0)
        high = weight.astype(jnp.bfloat16)
        low = (weight - high.astype(jnp.float32)).astype(jnp.bfloat16)
        rows = block[...]
        for part in (high, low):
            total = total + lax.dot_general(
                part, rows, (((0,), (0,)), ((), ())), preferred_element_type=jnp.float32
            )
    out_ref[...] = total.astype(jnp.bfloat16)


def combine(hops, ranks, logits, blocks):
    tokens, width = hops.shape[1], blocks[0].shape[1]
    return pl.pallas_call(
        combine_kernel,
        out_shape=jax.ShapeDtypeStruct((tokens, width), jnp.bfloat16),
        in_specs=[whole_vmem] * (3 + len(blocks)),
        out_specs=whole_vmem,
        cost_estimate=pl.CostEstimate(flops=4 * tokens * width * len(blocks) * blocks[0].shape[0], bytes_accessed=4 * tokens * width, transcendentals=0),
        name="combine",
    )(hops, ranks, logits, *blocks)


def expert_kernel(count, up_steps, *refs):
    inputs = refs[:count]
    gate_ref, up_ref, down_ref = refs[count : count + 3]
    outputs = refs[count + 3 : 2 * count + 3]
    hidden_ref = refs[-1]
    step = pl.program_id(0)
    rows = inputs[0].shape[0]
    tile = gate_ref.shape[1]

    @pl.when(step < up_steps)
    def _():
        x = jnp.concatenate([ref[...] for ref in inputs], axis=0)
        both = jnp.concatenate([gate_ref[...], up_ref[...]], axis=1)
        product = jnp.dot(x, both, preferred_element_type=jnp.float32)
        gate_part, up_part = product[:, :tile], product[:, tile:]
        hidden = gate_part / (1.0 + jnp.exp(-gate_part)) * up_part
        hidden_ref[:, pl.ds(pl.multiple_of(step * tile, tile), tile)] = hidden.astype(jnp.bfloat16)

    @pl.when(step >= up_steps)
    def _():
        product = jnp.dot(hidden_ref[...], down_ref[...], preferred_element_type=jnp.float32)
        for index, ref in enumerate(outputs):
            ref[...] = product[index * rows : (index + 1) * rows].astype(jnp.bfloat16)


def expert(blocks, gate, up, down):
    count = len(blocks)
    rows, width = blocks[0].shape
    units = gate.shape[1]
    tile = 128
    wide = min(512, width)
    up_steps, down_steps = units // tile, width // wide
    up_at = lambda i: (0, jnp.minimum(i, up_steps - 1))
    down_at = lambda i: (0, jnp.maximum(i - up_steps, 0))
    return pl.pallas_call(
        functools.partial(expert_kernel, count, up_steps),
        grid=(up_steps + down_steps,),
        out_shape=[jax.ShapeDtypeStruct((rows, width), jnp.bfloat16)] * count,
        in_specs=[pl.BlockSpec((rows, width), lambda i: (0, 0))] * count
        + [pl.BlockSpec((width, tile), up_at)] * 2
        + [pl.BlockSpec((units, wide), down_at)],
        out_specs=[pl.BlockSpec((rows, wide), down_at)] * count,
        scratch_shapes=[pltpu.VMEM((count * rows, units), jnp.bfloat16)],
        compiler_params=pltpu.CompilerParams(
            dimension_semantics=("arbitrary",), vmem_limit_bytes=vmem_bytes
        ),
        cost_estimate=pl.CostEstimate(
            flops=6 * count * rows * width * units,
            bytes_accessed=6 * width * units + 4 * count * rows * width,
            transcendentals=count * rows * units,
        ),
        name="expert",
    )(*blocks, gate, up, down)


def attention_kernel(heads, head_size, value_size, count, lam_ref, gain_ref, q_ref, *refs):
    blocks, out_ref = refs[:count], refs[count]
    score_ref, value_ref = refs[count + 1 :]
    rows = q_ref.shape[0]
    keys = blocks[0].shape[0]
    pair = 2 * head_size
    scale = head_size ** (-0.5)
    lanes = lax.broadcasted_iota(jnp.int32, (rows, pair), 1)

    for head in range(heads):
        first_value = heads * pair + head * value_size
        q = q_ref[:, head * pair : (head + 1) * pair].astype(jnp.float32) * scale
        q = jnp.concatenate(
            [jnp.where(lanes < head_size, q, 0.0), jnp.where(lanes < head_size, 0.0, q)], axis=0
        ).astype(jnp.bfloat16)

        @pl.when(pl.program_id(0) == 0)
        def _():
            for index, block in enumerate(blocks):
                value_ref[head, index * keys : (index + 1) * keys, :value_size] = block[
                    :, first_value : first_value + value_size
                ]
                value_ref[head, index * keys : (index + 1) * keys, value_size:] = jnp.ones(
                    (keys, value_size), jnp.bfloat16
                )

        peak = jnp.full((2 * rows, 128), -jnp.inf, jnp.float32)
        for index, block in enumerate(blocks):
            scores = lax.dot_general(
                q,
                block[:, head * pair : (head + 1) * pair],
                (((1,), (1,)), ((), ())),
                preferred_element_type=jnp.float32,
            )
            score_ref[:, index * keys : (index + 1) * keys] = scores
            for part in range(keys // 128):
                peak = jnp.maximum(peak, scores[:, part * 128 : (part + 1) * 128])
        maxima = jnp.max(peak, axis=1, keepdims=True)
        total = jnp.zeros((2 * rows, 2 * value_size), jnp.float32)
        for index in range(count):
            weights = jnp.exp(score_ref[:, index * keys : (index + 1) * keys] - maxima)
            total = total + jnp.dot(
                weights.astype(jnp.bfloat16),
                value_ref[head, index * keys : (index + 1) * keys, :],
                preferred_element_type=jnp.float32,
            )
        maps = total[:, :value_size] / total[:, value_size:]
        head_out = maps[:rows] - lam_ref[head] * maps[rows:]
        mean_square = jnp.mean(head_out * head_out, axis=-1, keepdims=True)
        out_ref[:, head * value_size : (head + 1) * value_size] = (
            head_out * lax.rsqrt(mean_square + epsilon) * gain_ref[...] * (1.0 - init_lambda)
        ).astype(jnp.bfloat16)


def attention(lam, gain, q, blocks):
    heads = lam.shape[0]
    value_size = gain.shape[0]
    head_size = q.shape[1] // (2 * heads)
    queries = q.shape[0]
    keys = blocks[0].shape[0]
    total_keys = keys * len(blocks)
    rows = min(256, queries)
    while rows > 16 and 8 * rows * total_keys > 2**23:
        rows //= 2
    return pl.pallas_call(
        functools.partial(attention_kernel, heads, head_size, value_size, len(blocks)),
        grid=(queries // rows,),
        out_shape=jax.ShapeDtypeStruct((queries, heads * value_size), jnp.bfloat16),
        in_specs=[
            pl.BlockSpec(memory_space=pltpu.SMEM),
            pl.BlockSpec((1, value_size), lambda i: (0, 0)),
            pl.BlockSpec((rows, q.shape[1]), lambda i: (i, 0)),
        ]
        + [pl.BlockSpec(blocks[0].shape, lambda i: (0, 0))] * len(blocks),
        out_specs=pl.BlockSpec((rows, heads * value_size), lambda i: (i, 0)),
        scratch_shapes=[
            pltpu.VMEM((2 * rows, total_keys), jnp.float32),
            pltpu.VMEM((heads, total_keys, 2 * value_size), jnp.bfloat16),
        ],
        compiler_params=pltpu.CompilerParams(
            dimension_semantics=("arbitrary",), vmem_limit_bytes=vmem_bytes
        ),
        cost_estimate=pl.CostEstimate(
            flops=heads * queries * total_keys * 2 * 2 * (head_size + value_size) * 2,
            bytes_accessed=2 * total_keys * heads * (2 * head_size + value_size),
            transcendentals=2 * heads * queries * total_keys,
        ),
        name="attention",
    )(lam, gain.reshape(1, -1), q, *blocks)


def gather_tp(block):
    size = lax.axis_size("tp")
    held = {0: block}
    bit = size // 2
    while bit:
        for index in list(held):
            held[index ^ bit] = swap(held[index], "tp", bit)
        bit //= 2
    return [held[i] for i in range(size)]


def scatter_tp(blocks):
    held = dict(enumerate(blocks))
    bit = 1
    while bit < len(blocks):
        sent = [i for i in sorted(held, reverse=True) if i & bit]
        for index in sent:
            came = swap(held.pop(index), "tp", bit)
            held[index ^ bit] = (
                held[index ^ bit].astype(jnp.float32) + came.astype(jnp.float32)
            ).astype(jnp.bfloat16)
        bit *= 2
    return held[0]


def per_device(
    queries,
    key_rows,
    value_rows,
    lambdas,
    head_gain,
    out_weight,
    moe_input,
    moe_gain,
    routes,
    route_logits,
    expert_gate,
    expert_up,
    expert_down,
):
    ep, tp = lax.axis_size("ep"), lax.axis_size("tp")
    me, column = lax.axis_index("ep"), lax.axis_index("tp")
    far = ep // 2
    tokens, top_count = routes.shape
    cap = capacity(tokens, top_count, ep)

    hops = jnp.bitwise_xor(routes.T, me)
    ranks, outgoing = dispatch(moe_input, moe_gain, hops, cap, ep)
    quarter = ep // 4
    groups = [range(0, far), range(far, far + quarter), range(far + quarter, ep)]

    local_rows, local_heads = queries.shape[0], lambdas.shape[0]
    half = local_heads // 2
    mine = (me // far).astype(jnp.int32)

    def halves(array):
        width = array.shape[1] // 2
        first, second = array[:, :width], array[:, width:]
        keep = jnp.where(mine == 0, first, second)
        give = jnp.where(mine == 0, second, first)
        return keep, give

    parts = local_rows // tp
    order = jnp.bitwise_xor(jnp.arange(tp, dtype=jnp.int32), column)
    query_blocks = queries.reshape(tp, parts, -1)
    ordered = jnp.concatenate(
        [lax.dynamic_index_in_dim(query_blocks, order[b], 0, keepdims=False) for b in range(tp)], axis=0
    )
    q_keep, q_give = halves(ordered)
    k_keep, k_give = halves(key_rows)
    v_keep, v_give = halves(value_rows)
    lam = jnp.where(mine == 0, lambdas[:half], lambdas[half:])
    kept = jnp.concatenate([k_keep, v_keep], axis=1)
    given = jnp.concatenate([k_give, v_give, q_give], axis=1)
    came = swap(given, "ep", far)
    kv_width = kept.shape[1]
    came_kv, came_q = came[:, :kv_width], came[:, kv_width:]
    key_blocks = [kept] + [swap(kept, "ep", k) for k in range(1, far)]
    key_blocks += [came_kv] + [swap(came_kv, "ep", k) for k in range(1, far)]

    arrived = {0: outgoing[0]}
    for group in (groups[1], groups[0], groups[2]):
        for k in group:
            if k:
                arrived[k] = swap(outgoing[k], "ep", k)

    attended = attention(lam, head_gain, jnp.concatenate([q_keep, came_q], axis=0), key_blocks)
    returned = swap(attended[local_rows:], "ep", far)
    kept_out = attended[:local_rows]
    both_heads = jnp.where(
        mine == 0,
        jnp.concatenate([kept_out, returned], axis=1),
        jnp.concatenate([returned, kept_out], axis=1),
    )
    mixer_blocks = [
        jnp.dot(
            both_heads[b * parts : (b + 1) * parts], out_weight, preferred_element_type=jnp.float32
        ).astype(jnp.bfloat16)
        for b in range(tp)
    ]

    replies = {}
    for group in groups:
        block = jnp.concatenate([arrived[k] for k in group], axis=0)
        partial = expert(gather_tp(block), expert_gate[0], expert_up[0], expert_down[0])
        summed = scatter_tp(partial)
        for index, k in enumerate(group):
            piece = summed[index * cap : (index + 1) * cap]
            replies[k] = swap(piece, "ep", k) if k else piece
    mixer_out = scatter_tp(mixer_blocks)
    expert_out = combine(hops, ranks, route_logits.T, [replies[k] for k in range(ep)])
    return (mixer_out, expert_out)


def solution(mesh):
    placed = (
        P("ep", "tp"),
        P("ep", "tp"),
        P("ep", "tp"),
        P("tp"),
        P(),
        P("tp", None),
        P(("ep", "tp"), None),
        P(),
        P(("ep", "tp"), None),
        P(("ep", "tp"), None),
        P("ep", None, "tp"),
        P("ep", None, "tp"),
        P("ep", "tp", None),
    )
    return jax.shard_map(
        per_device,
        mesh=mesh,
        in_specs=placed,
        out_specs=(P(("ep", "tp"), None), P(("ep", "tp"), None)),
        check_vma=False,
    )
```

```python
import functools

import jax
import jax.numpy as jnp
from jax import lax
from jax.experimental import pallas as pl
from jax.experimental.pallas import tpu as pltpu
from jax.sharding import PartitionSpec as P


epsilon = 1e-06
init_lambda = 0.2
small_vmem = 12 * 1024 * 1024
expert_vmem = 24 * 1024 * 1024
attention_vmem = 32 * 1024 * 1024


whole_vmem = pl.BlockSpec(memory_space=pltpu.VMEM)


def capacity(tokens, top_count, experts):
    return max(2, (top_count * tokens * 5 + 4 * experts - 1) // (4 * experts))


def swap(array, axis, mask):
    size = lax.axis_size(axis)
    return lax.ppermute(array, axis, [(i, i ^ mask) for i in range(size)])


def dispatch_kernel(cap, x_ref, gain_ref, hops_ref, ranks_ref, *blocks):
    tokens, _ = x_ref.shape
    rows = x_ref[...].astype(jnp.float32)
    mean_square = jnp.mean(rows * rows, axis=-1, keepdims=True)
    normed = (rows * lax.rsqrt(mean_square + epsilon) * gain_ref[...]).astype(jnp.bfloat16)
    count = len(blocks)
    top = hops_ref.shape[0]
    earlier = lax.broadcasted_iota(jnp.int32, (tokens, tokens), 0)
    later = lax.broadcasted_iota(jnp.int32, (tokens, tokens), 1)
    before = (earlier < later).astype(jnp.float32).astype(jnp.bfloat16)
    hop_ids = lax.broadcasted_iota(jnp.int32, (count, tokens), 0)
    base = jnp.zeros((count, 1), jnp.float32)
    ranks = []
    for j in range(top):
        chosen = (hops_ref[j : j + 1, :] == hop_ids).astype(jnp.float32)
        prefix = jnp.dot(chosen.astype(jnp.bfloat16), before, preferred_element_type=jnp.float32)
        rank = jnp.sum(chosen * (prefix + base), axis=0, keepdims=True)
        base = base + jnp.sum(chosen, axis=1, keepdims=True)
        ranks.append(rank.astype(jnp.int32))
        ranks_ref[j : j + 1, :] = ranks[-1]
    places = lax.broadcasted_iota(jnp.int32, (cap, tokens), 0)
    picks = []
    for k in range(count):
        picked = jnp.zeros((cap, tokens), jnp.float32)
        for j in range(top):
            hit = (hops_ref[j : j + 1, :] == k) & (ranks[j] == places)
            picked = picked + hit.astype(jnp.float32)
        picks.append(picked)
    picks = jnp.concatenate(picks, axis=0).astype(jnp.bfloat16)
    rows = jnp.dot(picks, normed, preferred_element_type=jnp.float32)
    for k, block in enumerate(blocks):
        block[...] = rows[k * cap : (k + 1) * cap].astype(jnp.bfloat16)


def dispatch(moe_input, moe_gain, hops, cap, count):
    tokens, width = moe_input.shape
    shapes = [jax.ShapeDtypeStruct(hops.shape, jnp.int32)]
    shapes += [jax.ShapeDtypeStruct((cap, width), jnp.bfloat16)] * count
    out = pl.pallas_call(
        functools.partial(dispatch_kernel, cap),
        out_shape=shapes,
        in_specs=[whole_vmem] * 3,
        out_specs=[whole_vmem] * len(shapes),
        cost_estimate=pl.CostEstimate(flops=2 * cap * count * tokens * width, bytes_accessed=4 * tokens * width, transcendentals=0),
        compiler_params=pltpu.CompilerParams(vmem_limit_bytes=small_vmem),
        name="dispatch",
    )(moe_input, moe_gain.reshape(1, -1), hops)
    return out[0], list(out[1:])


def window_kernel(ranks_ref, gate_ref, up_ref, down_ref, out_ref):
    out_ref[...] = ranks_ref[...]


def window(ranks, *weights):
    return pl.pallas_call(
        window_kernel,
        out_shape=jax.ShapeDtypeStruct(ranks.shape, ranks.dtype),
        in_specs=[whole_vmem] * (1 + len(weights)),
        out_specs=whole_vmem,
        compiler_params=pltpu.CompilerParams(vmem_limit_bytes=small_vmem),
        cost_estimate=pl.CostEstimate(flops=1, bytes_accessed=4 * ranks.size, transcendentals=0),
        name="window",
    )(ranks, *weights)


def combine_kernel(hops_ref, ranks_ref, logits_ref, *refs):
    blocks, out_ref = refs[:-1], refs[-1]
    top, tokens = hops_ref.shape
    cap = blocks[0].shape[0]
    logits = logits_ref[...]
    peak = jnp.max(logits, axis=0, keepdims=True)
    raised = jnp.exp(logits - peak)
    gates = raised / jnp.sum(raised, axis=0, keepdims=True)
    places = lax.broadcasted_iota(jnp.int32, (cap, tokens), 0)
    parts = []
    for k in range(len(blocks)):
        weight = jnp.zeros((cap, tokens), jnp.float32)
        for j in range(top):
            hit = (hops_ref[j : j + 1, :] == k) & (ranks_ref[j : j + 1, :] == places)
            weight = weight + jnp.where(hit, gates[j : j + 1, :], 0.0)
        parts.append(weight)
    weights = jnp.concatenate(parts, axis=0)
    high = weights.astype(jnp.bfloat16)
    low = (weights - high.astype(jnp.float32)).astype(jnp.bfloat16)
    rows = jnp.concatenate([block[...] for block in blocks], axis=0)
    both = lax.dot_general(
        jnp.concatenate([high, low], axis=1),
        rows,
        (((0,), (0,)), ((), ())),
        preferred_element_type=jnp.float32,
    )
    out_ref[...] = (both[:tokens] + both[tokens:]).astype(jnp.bfloat16)


def combine(hops, ranks, logits, blocks):
    tokens, width = hops.shape[1], blocks[0].shape[1]
    return pl.pallas_call(
        combine_kernel,
        out_shape=jax.ShapeDtypeStruct((tokens, width), jnp.bfloat16),
        in_specs=[whole_vmem] * (3 + len(blocks)),
        out_specs=whole_vmem,
        cost_estimate=pl.CostEstimate(flops=4 * tokens * width * len(blocks) * blocks[0].shape[0], bytes_accessed=4 * tokens * width, transcendentals=0),
        compiler_params=pltpu.CompilerParams(vmem_limit_bytes=small_vmem),
        name="combine",
    )(hops, ranks, logits, *blocks)


def expert_kernel(count, *refs):
    inputs = refs[:count]
    gate_ref, up_ref, down_ref = refs[count : count + 3]
    outputs = refs[count + 3 : -1]
    hidden_ref = refs[-1]
    _, width = inputs[0].shape
    tile, wide = 128, min(512, width)
    order = list(range(0, count, 2)) + list(range(1, count, 2))

    def hidden_step(step, carry):
        at = pl.ds(pl.multiple_of(step * tile, tile), tile)
        x = jnp.concatenate([inputs[i][...] for i in order], axis=0)
        both = jnp.concatenate([gate_ref[:, at], up_ref[:, at]], axis=1)
        product = jnp.dot(x, both, preferred_element_type=jnp.float32)
        gate_part, up_part = product[:, :tile], product[:, tile:]
        hidden = gate_part / (1.0 + jnp.exp(-gate_part)) * up_part
        hidden_ref[:, at] = hidden.astype(jnp.bfloat16)
        return carry

    def down_step(step, carry):
        at = pl.ds(pl.multiple_of(step * wide, wide), wide)
        product = jnp.dot(hidden_ref[...], down_ref[:, at], preferred_element_type=jnp.float32)
        first = 0
        for ref in outputs:
            ref[:, at] = product[first : first + ref.shape[0]].astype(jnp.bfloat16)
            first += ref.shape[0]
        return carry

    lax.fori_loop(0, gate_ref.shape[1] // tile, hidden_step, 0)
    lax.fori_loop(0, width // wide, down_step, 0)


def expert(blocks, gate, up, down):
    count = len(blocks)
    rows, width = blocks[0].shape
    units = gate.shape[1]
    stay = count - count // 2
    shapes = [jax.ShapeDtypeStruct((rows, width), jnp.bfloat16)] * stay
    shapes += [jax.ShapeDtypeStruct((rows * (count // 2), width), jnp.bfloat16)]
    return pl.pallas_call(
        functools.partial(expert_kernel, count),
        out_shape=shapes,
        in_specs=[whole_vmem] * (count + 3),
        out_specs=[whole_vmem] * len(shapes),
        scratch_shapes=[pltpu.VMEM((count * rows, units), jnp.bfloat16)],
        compiler_params=pltpu.CompilerParams(vmem_limit_bytes=expert_vmem),
        cost_estimate=pl.CostEstimate(
            flops=6 * count * rows * width * units,
            bytes_accessed=6 * width * units + 4 * count * rows * width,
            transcendentals=count * rows * units,
        ),
    )(*blocks, gate, up, down)


def attention_kernel(heads, head_size, value_size, rows, count, mine_ref, lam_ref, gain_ref, q_ref, *refs):
    blocks, out_ref = refs[:count], refs[count]
    value_ref, score_a, score_b, peak_a, peak_b = refs[count + 1 :]
    tiles = q_ref.shape[0] // rows
    keys = blocks[0].shape[0]
    pair = 2 * head_size
    scale = head_size ** (-0.5)
    lanes = lax.broadcasted_iota(jnp.int32, (rows, pair), 1)

    for head in range(heads):
        lam = lam_ref[mine_ref[0] * heads + head]
        first_value = heads * pair + head * value_size

        for index, block in enumerate(blocks):
            at = slice(index * keys, (index + 1) * keys)
            value_ref[at, :value_size] = block[:, first_value : first_value + value_size]
            value_ref[at, value_size:] = jnp.ones((keys, value_size), jnp.bfloat16)

        def step(following, score_to, peak_to, current, score_from, peak_from):
            at = pl.ds(pl.multiple_of(following * rows, rows), rows)
            q = q_ref[at, head * pair : (head + 1) * pair].astype(jnp.float32) * scale
            q = jnp.concatenate(
                [jnp.where(lanes < head_size, q, 0.0), jnp.where(lanes < head_size, 0.0, q)], axis=0
            ).astype(jnp.bfloat16)
            peak = jnp.full((2 * rows, 128), -jnp.inf, jnp.float32)
            if current is not None:
                maxima = jnp.concatenate([peak_from[...]] * (keys // 128), axis=1)
                total = jnp.zeros((2 * rows, 2 * value_size), jnp.float32)
            for index, block in enumerate(blocks):
                columns = slice(index * keys, (index + 1) * keys)
                scores = lax.dot_general(
                    q,
                    block[:, head * pair : (head + 1) * pair],
                    (((1,), (1,)), ((), ())),
                    preferred_element_type=jnp.float32,
                )
                score_to[:, columns] = scores
                for part in range(keys // 128):
                    peak = jnp.maximum(peak, scores[:, part * 128 : (part + 1) * 128])
                if current is not None:
                    weights = jnp.exp(score_from[:, columns] - maxima)
                    total = total + jnp.dot(
                        weights.astype(jnp.bfloat16),
                        value_ref[columns, :],
                        preferred_element_type=jnp.float32,
                    )
            peak_to[...] = jnp.broadcast_to(jnp.max(peak, axis=1, keepdims=True), peak.shape)
            if current is not None:
                maps = total[:, :value_size] / total[:, value_size:]
                head_out = maps[:rows] - lam * maps[rows:]
                mean_square = jnp.mean(head_out * head_out, axis=-1, keepdims=True)
                normal = head_out * lax.rsqrt(mean_square + epsilon) * gain_ref[...] * (1.0 - init_lambda)
                out_at = pl.ds(pl.multiple_of(current * rows, rows), rows)
                out_ref[out_at, head * value_size : (head + 1) * value_size] = normal.astype(jnp.bfloat16)

        step(0, score_a, peak_a, None, None, None)

        def two_tiles(i, carry):
            step(2 * i + 1, score_b, peak_b, 2 * i, score_a, peak_a)
            step(jnp.minimum(2 * i + 2, tiles - 1), score_a, peak_a, 2 * i + 1, score_b, peak_b)
            return carry

        lax.fori_loop(0, tiles // 2, two_tiles, 0)


def attention(mine, lam, gain, q, blocks, heads):
    value_size = gain.shape[0]
    head_size = q.shape[1] // (2 * heads)
    queries = q.shape[0]
    keys = blocks[0].shape[0]
    total_keys = keys * len(blocks)
    rows = min(256, queries // 2)
    while rows > 16 and 8 * rows * total_keys > 2**23:
        rows //= 2
    smem = pl.BlockSpec(memory_space=pltpu.SMEM)
    return pl.pallas_call(
        functools.partial(attention_kernel, heads, head_size, value_size, rows, len(blocks)),
        out_shape=jax.ShapeDtypeStruct((queries, heads * value_size), jnp.bfloat16),
        in_specs=[smem, smem] + [whole_vmem] * (2 + len(blocks)),
        out_specs=whole_vmem,
        scratch_shapes=[pltpu.VMEM((total_keys, 2 * value_size), jnp.bfloat16)]
        + [pltpu.VMEM((2 * rows, total_keys), jnp.float32)] * 2
        + [pltpu.VMEM((2 * rows, 128), jnp.float32)] * 2,
        compiler_params=pltpu.CompilerParams(vmem_limit_bytes=attention_vmem),
        cost_estimate=pl.CostEstimate(
            flops=heads * queries * total_keys * 2 * 2 * (head_size + value_size) * 2,
            bytes_accessed=2 * total_keys * heads * (2 * head_size + value_size),
            transcendentals=2 * heads * queries * total_keys,
        ),
    )(mine.reshape(1), lam, gain.reshape(1, -1), q, *blocks)


def mixer_kernel(count, mine_ref, *refs):
    columns, weights, out_ref = refs[:count], refs[count:-1], refs[-1]
    half = columns[0].shape[1] // 2
    first = mine_ref[0] == 0
    ordered = []
    for ref in columns:
        kept, other = ref[:, :half], ref[:, half:]
        ordered += [jnp.where(first, kept, other), jnp.where(first, other, kept)]
    out_ref[...] = jnp.dot(
        jnp.concatenate(ordered, axis=1),
        jnp.concatenate([ref[...] for ref in weights], axis=0),
        preferred_element_type=jnp.float32,
    ).astype(jnp.bfloat16)


def mixer(mine, columns, weights):
    rows, width = columns[0].shape[0], weights[0].shape[1]
    return pl.pallas_call(
        functools.partial(mixer_kernel, len(columns)),
        out_shape=jax.ShapeDtypeStruct((rows, width), jnp.bfloat16),
        in_specs=[pl.BlockSpec(memory_space=pltpu.SMEM)] + [whole_vmem] * (len(columns) + len(weights)),
        out_specs=whole_vmem,
        compiler_params=pltpu.CompilerParams(vmem_limit_bytes=expert_vmem),
        cost_estimate=pl.CostEstimate(
            flops=2 * rows * width * sum(w.shape[0] for w in weights),
            bytes_accessed=2 * width * sum(w.shape[0] for w in weights),
            transcendentals=0,
        ),
        name="mixer",
    )(mine.reshape(1), *columns, *weights)


def gather_all(block, axis, size):
    held = {0: block}
    bit = size // 2
    while bit:
        for index in list(held):
            held[index ^ bit] = swap(held[index], axis, bit)
        bit //= 2
    return [held[i] for i in range(size)]


def scatter_tp(stay, sent):
    came = swap(sent, "tp", 1)
    rows = stay[0].shape[0]
    held = {}
    for i in reversed(range(len(stay))):
        held[2 * i] = add_rounded(stay[i], came[i * rows : (i + 1) * rows])
    bit = 2
    while bit < 2 * len(stay):
        for index in [i for i in sorted(held, reverse=True) if i & bit]:
            came = swap(held.pop(index), "tp", bit)
            held[index ^ bit] = add_rounded(held[index ^ bit], came)
        bit *= 2
    return held[0]


def add_rounded(first, second):
    return (first.astype(jnp.float32) + second.astype(jnp.float32)).astype(jnp.bfloat16)


def per_device(
    queries,
    key_rows,
    value_rows,
    lambdas,
    head_gain,
    out_weight,
    moe_input,
    moe_gain,
    routes,
    route_logits,
    expert_gate,
    expert_up,
    expert_down,
):
    ep, tp = lax.axis_size("ep"), lax.axis_size("tp")
    me, column = lax.axis_index("ep"), lax.axis_index("tp")
    far = ep // 2
    tokens, top_count = routes.shape
    cap = capacity(tokens, top_count, ep)

    hops = jnp.bitwise_xor(routes.T, me)
    ranks, outgoing = dispatch(moe_input, moe_gain, hops, cap, ep)
    ranks = window(ranks, expert_gate[0], expert_up[0], expert_down[0])
    quarter = ep // 4
    groups = [range(0, far), range(far, far + quarter), range(far + quarter, ep)]

    local_rows, local_heads = queries.shape[0], lambdas.shape[0]
    half = local_heads // 2
    mine = (me // far).astype(jnp.int32)

    def halves(array):
        width = array.shape[1] // 2
        first, second = array[:, :width], array[:, width:]
        keep = jnp.where(mine == 0, first, second)
        give = jnp.where(mine == 0, second, first)
        return keep, give

    parts = local_rows // tp
    ordered = jnp.concatenate(
        [
            lax.dynamic_slice_in_dim(queries, jnp.bitwise_xor(column, b) * parts, parts, 0)
            for b in range(tp)
        ],
        axis=0,
    )
    q_keep, q_give = halves(ordered)
    k_keep, k_give = halves(key_rows)
    v_keep, v_give = halves(value_rows)
    kept = jnp.concatenate([k_keep, v_keep], axis=1)
    given = jnp.concatenate([k_give, v_give, q_give], axis=1)
    came = swap(given, "ep", far)
    kv_width = kept.shape[1]
    came_kv, came_q = came[:, :kv_width], came[:, kv_width:]
    key_blocks = gather_all(kept, "ep", far) + gather_all(came_kv, "ep", far)

    arrived = {0: outgoing[0]}
    for group in (groups[1], groups[0], groups[2]):
        for k in group:
            if k:
                arrived[k] = swap(outgoing[k], "ep", k)

    sent_out = attention(mine, lambdas, head_gain, came_q, key_blocks, half)
    returned = swap(sent_out, "ep", far)
    kept_out = attention(mine, lambdas, head_gain, q_keep, key_blocks, half)
    both = jnp.concatenate([kept_out, returned], axis=1)
    moved = [both[b * parts : (b + 1) * parts] for b in range(tp)]
    moved = [swap(block, "tp", b) if b else block for b, block in enumerate(moved)]
    half_rows = out_weight.shape[0] // 2
    first_rows = gather_all(out_weight[:half_rows], "tp", tp)
    last_rows = gather_all(out_weight[half_rows:], "tp", tp)
    mixer_out = mixer(mine, moved, [w for pair in zip(first_rows, last_rows) for w in pair])

    replies = {}
    for group in groups:
        block = jnp.concatenate([arrived[k] for k in group], axis=0)
        blocks = gather_all(block, "tp", tp)
        partial = expert(blocks, expert_gate[0], expert_up[0], expert_down[0])
        summed = scatter_tp(partial[:-1], partial[-1])
        for index, k in enumerate(group):
            piece = summed[index * cap : (index + 1) * cap]
            replies[k] = swap(piece, "ep", k) if k else piece
    expert_out = combine(hops, ranks, route_logits.T, [replies[k] for k in range(ep)])
    return (mixer_out, expert_out)


def solution(mesh):
    placed = (
        P("ep", "tp"),
        P("ep", "tp"),
        P("ep", "tp"),
        P("tp"),
        P(),
        P("tp", None),
        P(("ep", "tp"), None),
        P(),
        P(("ep", "tp"), None),
        P(("ep", "tp"), None),
        P("ep", None, "tp"),
        P("ep", None, "tp"),
        P("ep", "tp", None),
    )
    return jax.shard_map(
        per_device,
        mesh=mesh,
        in_specs=placed,
        out_specs=(P(("ep", "tp"), None), P(("ep", "tp"), None)),
        check_vma=False,
    )
```

```python
import functools

import jax
import jax.numpy as jnp
from jax import lax
from jax.experimental import pallas as pl
from jax.experimental.pallas import tpu as pltpu
from jax.sharding import PartitionSpec as P


epsilon = 1e-06
init_lambda = 0.2
small_vmem = 6 * 1024 * 1024
expert_vmem = 10 * 1024 * 1024
attention_margin = 3 * 1024 * 1024


whole_vmem = pl.BlockSpec(memory_space=pltpu.VMEM)


def capacity(tokens, top_count, experts):
    return max(2, (top_count * tokens * 5 + 4 * experts - 1) // (4 * experts))


def swap(array, axis, mask):
    size = lax.axis_size(axis)
    return lax.ppermute(array, axis, [(i, i ^ mask) for i in range(size)])


def dispatch_kernel(cap, place_ref, x_ref, gain_ref, routes_ref, hops_ref, ranks_ref, *blocks):
    tokens, _ = x_ref.shape
    rows = x_ref[...].astype(jnp.float32)
    mean_square = jnp.mean(rows * rows, axis=-1, keepdims=True)
    normed = (rows * lax.rsqrt(mean_square + epsilon) * gain_ref[...]).astype(jnp.bfloat16)
    count = len(blocks)
    top = routes_ref.shape[0]
    hops_ref[...] = routes_ref[...] ^ place_ref[0]
    earlier = lax.broadcasted_iota(jnp.int32, (tokens, tokens), 0)
    later = lax.broadcasted_iota(jnp.int32, (tokens, tokens), 1)
    before = (earlier < later).astype(jnp.float32).astype(jnp.bfloat16)
    hop_ids = lax.broadcasted_iota(jnp.int32, (count, tokens), 0)
    base = jnp.zeros((count, 1), jnp.float32)
    ranks = []
    for j in range(top):
        chosen = (hops_ref[j : j + 1, :] == hop_ids).astype(jnp.float32)
        prefix = jnp.dot(chosen.astype(jnp.bfloat16), before, preferred_element_type=jnp.float32)
        rank = jnp.sum(chosen * (prefix + base), axis=0, keepdims=True)
        base = base + jnp.sum(chosen, axis=1, keepdims=True)
        ranks.append(rank.astype(jnp.int32))
        ranks_ref[j : j + 1, :] = ranks[-1]
    places = lax.broadcasted_iota(jnp.int32, (cap, tokens), 0)
    picks = []
    for k in range(count):
        picked = jnp.zeros((cap, tokens), jnp.float32)
        for j in range(top):
            hit = (hops_ref[j : j + 1, :] == k) & (ranks[j] == places)
            picked = picked + hit.astype(jnp.float32)
        picks.append(picked)
    picks = jnp.concatenate(picks, axis=0).astype(jnp.bfloat16)
    rows = jnp.dot(picks, normed, preferred_element_type=jnp.float32)
    for k, block in enumerate(blocks):
        block[...] = rows[k * cap : (k + 1) * cap].astype(jnp.bfloat16)


def dispatch(place, moe_input, moe_gain, routes, cap, count):
    tokens, width = moe_input.shape
    shapes = [jax.ShapeDtypeStruct(routes.shape, jnp.int32)] * 2
    shapes += [jax.ShapeDtypeStruct((cap, width), jnp.bfloat16)] * count
    out = pl.pallas_call(
        functools.partial(dispatch_kernel, cap),
        out_shape=shapes,
        in_specs=[pl.BlockSpec(memory_space=pltpu.SMEM)] + [whole_vmem] * 3,
        out_specs=[whole_vmem] * len(shapes),
        cost_estimate=pl.CostEstimate(flops=2 * cap * count * tokens * width, bytes_accessed=4 * tokens * width, transcendentals=0),
        compiler_params=pltpu.CompilerParams(vmem_limit_bytes=small_vmem),
        name="dispatch",
    )(place, moe_input, moe_gain.reshape(1, -1), routes)
    return out[0], out[1], list(out[2:])


def pack_kernel(count, place_ref, q_ref, k_ref, v_ref, kept_ref, given_ref, q_keep_ref):
    first = place_ref[2] == 0
    parts = q_ref.shape[0] // count
    k_half, v_half = k_ref.shape[1] // 2, v_ref.shape[1] // 2

    def halves(array):
        width = array.shape[1] // 2
        low, high = array[:, :width], array[:, width:]
        return jnp.where(first, low, high), jnp.where(first, high, low)

    kept_ref[:, :k_half], given_ref[:, :k_half] = halves(k_ref[...])
    kept_ref[:, k_half:], given_ref[:, k_half : k_half + v_half] = halves(v_ref[...])
    for b in range(count):
        source = pl.ds(pl.multiple_of((place_ref[1] ^ b) * parts, parts), parts)
        at = slice(b * parts, (b + 1) * parts)
        q_keep_ref[at, :], given_ref[at, k_half + v_half :] = halves(q_ref[source, :])


def pack(place, queries, keys, values, count):
    rows = queries.shape[0]
    q_half, k_half, v_half = queries.shape[1] // 2, keys.shape[1] // 2, values.shape[1] // 2
    widths = (k_half + v_half, k_half + v_half + q_half, q_half)
    return pl.pallas_call(
        functools.partial(pack_kernel, count),
        out_shape=[jax.ShapeDtypeStruct((rows, width), jnp.bfloat16) for width in widths],
        in_specs=[pl.BlockSpec(memory_space=pltpu.SMEM)] + [whole_vmem] * 3,
        out_specs=[whole_vmem] * 3,
        compiler_params=pltpu.CompilerParams(vmem_limit_bytes=small_vmem),
        cost_estimate=pl.CostEstimate(flops=rows, bytes_accessed=8 * rows * widths[1], transcendentals=0),
        name="pack",
    )(place, queries, keys, values)


def window_kernel(ranks_ref, gate_ref, up_ref, down_ref, out_ref):
    out_ref[...] = ranks_ref[...]


def window(ranks, *weights):
    return pl.pallas_call(
        window_kernel,
        out_shape=jax.ShapeDtypeStruct(ranks.shape, ranks.dtype),
        in_specs=[whole_vmem] * (1 + len(weights)),
        out_specs=whole_vmem,
        compiler_params=pltpu.CompilerParams(vmem_limit_bytes=small_vmem),
        cost_estimate=pl.CostEstimate(flops=1, bytes_accessed=4 * ranks.size, transcendentals=0),
        name="window",
    )(ranks, *weights)


def combine_kernel(hops_ref, ranks_ref, logits_ref, *refs):
    blocks, out_ref = refs[:-1], refs[-1]
    top, tokens = hops_ref.shape
    cap = blocks[0].shape[0]
    logits = logits_ref[...]
    peak = jnp.max(logits, axis=0, keepdims=True)
    raised = jnp.exp(logits - peak)
    gates = raised / jnp.sum(raised, axis=0, keepdims=True)
    places = lax.broadcasted_iota(jnp.int32, (cap, tokens), 0)
    parts = []
    for k in range(len(blocks)):
        weight = jnp.zeros((cap, tokens), jnp.float32)
        for j in range(top):
            hit = (hops_ref[j : j + 1, :] == k) & (ranks_ref[j : j + 1, :] == places)
            weight = weight + jnp.where(hit, gates[j : j + 1, :], 0.0)
        parts.append(weight)
    weights = jnp.concatenate(parts, axis=0)
    high = weights.astype(jnp.bfloat16)
    low = (weights - high.astype(jnp.float32)).astype(jnp.bfloat16)
    rows = jnp.concatenate([block[...] for block in blocks], axis=0)
    both = lax.dot_general(
        jnp.concatenate([high, low], axis=1),
        rows,
        (((0,), (0,)), ((), ())),
        preferred_element_type=jnp.float32,
    )
    out_ref[...] = (both[:tokens] + both[tokens:]).astype(jnp.bfloat16)


def combine(hops, ranks, logits, blocks):
    tokens, width = hops.shape[1], blocks[0].shape[1]
    return pl.pallas_call(
        combine_kernel,
        out_shape=jax.ShapeDtypeStruct((tokens, width), jnp.bfloat16),
        in_specs=[whole_vmem] * (3 + len(blocks)),
        out_specs=whole_vmem,
        cost_estimate=pl.CostEstimate(flops=4 * tokens * width * len(blocks) * blocks[0].shape[0], bytes_accessed=4 * tokens * width, transcendentals=0),
        compiler_params=pltpu.CompilerParams(vmem_limit_bytes=small_vmem),
        name="combine",
    )(hops, ranks, logits, *blocks)


def expert_kernel(count, *refs):
    inputs = refs[:count]
    gate_ref, up_ref, down_ref = refs[count : count + 3]
    outputs = refs[count + 3 : -1]
    hidden_ref = refs[-1]
    rows, width = inputs[0].shape
    tile, wide = 128, min(512, width)
    order = list(range(0, count, 2)) + list(range(1, count, 2))

    def hidden_step(step, carry):
        at = pl.ds(pl.multiple_of(step * tile, tile), tile)
        x = jnp.concatenate([inputs[i][...] for i in order], axis=0)
        both = jnp.concatenate([gate_ref[:, at], up_ref[:, at]], axis=1)
        product = jnp.dot(x, both, preferred_element_type=jnp.float32)
        gate_part, up_part = product[:, :tile], product[:, tile:]
        hidden = gate_part / (1.0 + jnp.exp(-gate_part)) * up_part
        hidden_ref[:, at] = hidden.astype(jnp.bfloat16)
        return carry

    def down_step(step, carry):
        at = pl.ds(pl.multiple_of(step * wide, wide), wide)
        product = jnp.dot(hidden_ref[...], down_ref[:, at], preferred_element_type=jnp.float32)
        first = 0
        for ref in outputs:
            ref[:, at] = product[first : first + ref.shape[0]].astype(jnp.bfloat16)
            first += ref.shape[0]
        return carry

    short = count * rows <= 512
    lax.fori_loop(0, gate_ref.shape[1] // tile, hidden_step, 0, unroll=short)
    lax.fori_loop(0, width // wide, down_step, 0, unroll=short)


def expert(blocks, gate, up, down):
    count = len(blocks)
    rows, width = blocks[0].shape
    units = gate.shape[1]
    stay = count - count // 2
    shapes = [jax.ShapeDtypeStruct((rows, width), jnp.bfloat16)] * stay
    shapes += [jax.ShapeDtypeStruct((rows * (count // 2), width), jnp.bfloat16)]
    return pl.pallas_call(
        functools.partial(expert_kernel, count),
        out_shape=shapes,
        in_specs=[whole_vmem] * (count + 3),
        out_specs=[whole_vmem] * len(shapes),
        scratch_shapes=[pltpu.VMEM((count * rows, units), jnp.bfloat16)],
        compiler_params=pltpu.CompilerParams(vmem_limit_bytes=expert_vmem),
        cost_estimate=pl.CostEstimate(
            flops=6 * count * rows * width * units,
            bytes_accessed=6 * width * units + 4 * count * rows * width,
            transcendentals=count * rows * units,
        ),
    )(*blocks, gate, up, down)


def attention_kernel(heads, head_size, value_size, rows, count, place_ref, lam_ref, gain_ref, q_ref, *refs):
    blocks, out_ref = refs[:count], refs[count]
    value_ref, score_a, score_b, peak_a, peak_b = refs[count + 1 :]
    tiles = q_ref.shape[0] // rows
    keys = blocks[0].shape[0]
    pair = 2 * head_size
    scale = head_size ** (-0.5)
    lanes = lax.broadcasted_iota(jnp.int32, (rows, pair), 1)

    for head in range(heads):
        lam = lam_ref[place_ref[2] * heads + head]
        first_value = heads * pair + head * value_size

        for index, block in enumerate(blocks):
            at = slice(index * keys, (index + 1) * keys)
            value_ref[at, :value_size] = block[:, first_value : first_value + value_size]
            value_ref[at, value_size:] = jnp.ones((keys, value_size), jnp.bfloat16)

        def step(following, score_to, peak_to, current, score_from, peak_from):
            if following is not None:
                at = pl.ds(pl.multiple_of(following * rows, rows), rows)
                q = q_ref[at, head * pair : (head + 1) * pair].astype(jnp.float32) * scale
                q = jnp.concatenate(
                    [jnp.where(lanes < head_size, q, 0.0), jnp.where(lanes < head_size, 0.0, q)], axis=0
                ).astype(jnp.bfloat16)
                peak = jnp.full((2 * rows, 128), -jnp.inf, jnp.float32)
            if current is not None:
                maxima = jnp.concatenate([peak_from[...]] * (keys // 128), axis=1)
                total = jnp.zeros((2 * rows, 2 * value_size), jnp.float32)
            for index, block in enumerate(blocks):
                columns = slice(index * keys, (index + 1) * keys)
                if following is not None:
                    scores = lax.dot_general(
                        q,
                        block[:, head * pair : (head + 1) * pair],
                        (((1,), (1,)), ((), ())),
                        preferred_element_type=jnp.float32,
                    )
                    score_to[:, columns] = scores
                    for part in range(keys // 128):
                        peak = jnp.maximum(peak, scores[:, part * 128 : (part + 1) * 128])
                if current is not None:
                    weights = jnp.exp(score_from[:, columns] - maxima)
                    total = total + jnp.dot(
                        weights.astype(jnp.bfloat16),
                        value_ref[columns, :],
                        preferred_element_type=jnp.float32,
                    )
            if following is not None:
                peak_to[...] = jnp.broadcast_to(jnp.max(peak, axis=1, keepdims=True), peak.shape)
            if current is not None:
                maps = total[:, :value_size] / total[:, value_size:]
                head_out = maps[:rows] - lam * maps[rows:]
                mean_square = jnp.mean(head_out * head_out, axis=-1, keepdims=True)
                normal = head_out * lax.rsqrt(mean_square + epsilon) * gain_ref[...] * (1.0 - init_lambda)
                out_at = pl.ds(pl.multiple_of(current * rows, rows), rows)
                out_ref[out_at, head * value_size : (head + 1) * value_size] = normal.astype(jnp.bfloat16)

        def two_tiles(i, carry):
            step(2 * i + 1, score_b, peak_b, 2 * i, score_a, peak_a)
            step(2 * i + 2, score_a, peak_a, 2 * i + 1, score_b, peak_b)
            return carry

        step(0, score_a, peak_a, None, None, None)
        if tiles > 2:
            lax.fori_loop(0, tiles // 2 - 1, two_tiles, 0)
        step(tiles - 1, score_b, peak_b, tiles - 2, score_a, peak_a)
        step(None, None, None, tiles - 1, score_b, peak_b)


def attention(place, lam, gain, q, blocks, heads):
    value_size = gain.shape[0]
    head_size = q.shape[1] // (2 * heads)
    queries = q.shape[0]
    keys = blocks[0].shape[0]
    total_keys = keys * len(blocks)
    rows = min(256, queries // 2)
    while rows > 16 and 8 * rows * total_keys > 2**23:
        rows //= 2
    smem = pl.BlockSpec(memory_space=pltpu.SMEM)
    scratch = 4 * total_keys * value_size + 16 * rows * (total_keys + 128)
    room = scratch + 2 * blocks[0].size * len(blocks) + attention_margin
    return pl.pallas_call(
        functools.partial(attention_kernel, heads, head_size, value_size, rows, len(blocks)),
        out_shape=jax.ShapeDtypeStruct((queries, heads * value_size), jnp.bfloat16),
        in_specs=[smem, smem] + [whole_vmem] * (2 + len(blocks)),
        out_specs=whole_vmem,
        scratch_shapes=[pltpu.VMEM((total_keys, 2 * value_size), jnp.bfloat16)]
        + [pltpu.VMEM((2 * rows, total_keys), jnp.float32)] * 2
        + [pltpu.VMEM((2 * rows, 128), jnp.float32)] * 2,
        compiler_params=pltpu.CompilerParams(vmem_limit_bytes=room),
        cost_estimate=pl.CostEstimate(
            flops=heads * queries * total_keys * 2 * 2 * (head_size + value_size) * 2,
            bytes_accessed=2 * total_keys * heads * (2 * head_size + value_size),
            transcendentals=2 * heads * queries * total_keys,
        ),
    )(place, lam, gain.reshape(1, -1), q, *blocks)


def mixer_kernel(count, place_ref, *refs):
    columns, weights, out_ref = refs[:count], refs[count:-1], refs[-1]
    half = columns[0].shape[1] // 2
    first = place_ref[2] == 0
    ordered = []
    for ref in columns:
        kept, other = ref[:, :half], ref[:, half:]
        ordered += [jnp.where(first, kept, other), jnp.where(first, other, kept)]
    out_ref[...] = jnp.dot(
        jnp.concatenate(ordered, axis=1),
        jnp.concatenate([ref[...] for ref in weights], axis=0),
        preferred_element_type=jnp.float32,
    ).astype(jnp.bfloat16)


def mixer(place, columns, weights):
    rows, width = columns[0].shape[0], weights[0].shape[1]
    return pl.pallas_call(
        functools.partial(mixer_kernel, len(columns)),
        out_shape=jax.ShapeDtypeStruct((rows, width), jnp.bfloat16),
        in_specs=[pl.BlockSpec(memory_space=pltpu.SMEM)] + [whole_vmem] * (len(columns) + len(weights)),
        out_specs=whole_vmem,
        compiler_params=pltpu.CompilerParams(vmem_limit_bytes=expert_vmem),
        cost_estimate=pl.CostEstimate(
            flops=2 * rows * width * sum(w.shape[0] for w in weights),
            bytes_accessed=2 * width * sum(w.shape[0] for w in weights),
            transcendentals=0,
        ),
        name="mixer",
    )(place, *columns, *weights)


def gather_all(block, axis, bits):
    held = {0: block}
    for bit in bits:
        for index in list(held):
            held[index ^ bit] = swap(held[index], axis, bit)
    return [held[i] for i in sorted(held)]


def bits_below(size):
    bits = []
    while size > 1:
        size //= 2
        bits.append(size)
    return bits


def key_bits(ep):
    return bits_below(ep)[:1] + bits_below(ep)[2:]


def scatter_tp(stay, sent):
    came = swap(sent, "tp", 1)
    rows = stay[0].shape[0]
    held = {}
    for i in reversed(range(len(stay))):
        held[2 * i] = add_rounded(stay[i], came[i * rows : (i + 1) * rows])
    bit = 2
    while bit < 2 * len(stay):
        for index in [i for i in sorted(held, reverse=True) if i & bit]:
            came = swap(held.pop(index), "tp", bit)
            held[index ^ bit] = add_rounded(held[index ^ bit], came)
        bit *= 2
    return held[0]


def add_rounded(first, second):
    return (first.astype(jnp.float32) + second.astype(jnp.float32)).astype(jnp.bfloat16)


def per_device(
    queries,
    key_rows,
    value_rows,
    lambdas,
    head_gain,
    out_weight,
    moe_input,
    moe_gain,
    routes,
    route_logits,
    expert_gate,
    expert_up,
    expert_down,
):
    ep, tp = lax.axis_size("ep"), lax.axis_size("tp")
    me, column = lax.axis_index("ep"), lax.axis_index("tp")
    far = ep // 2
    tokens, top_count = routes.shape
    cap = capacity(tokens, top_count, ep)

    partner = far // 2
    place = jnp.stack([me, column, (me // partner) % 2]).astype(jnp.int32)
    hops, ranks, outgoing = dispatch(place, moe_input, moe_gain, routes.T, cap, ep)
    ranks = window(ranks, expert_gate[0], expert_up[0], expert_down[0])
    quarter = ep // 4
    groups = [range(0, far), range(far, far + quarter), range(far + quarter, ep)]

    local_rows, local_heads = queries.shape[0], lambdas.shape[0]
    half = local_heads // 2
    kept, given, q_keep = pack(place, queries, key_rows, value_rows, tp)
    came = swap(given, "ep", partner)
    kv_width = kept.shape[1]
    parts = local_rows // tp
    came_kv, came_q = came[:, :kv_width], came[:, kv_width:]
    key_blocks = gather_all(kept, "ep", key_bits(ep)) + gather_all(came_kv, "ep", key_bits(ep))

    arrived = {0: outgoing[0]}
    for group in (groups[1], groups[0], groups[2]):
        for k in group:
            if k:
                arrived[k] = swap(outgoing[k], "ep", k)

    sent_out = attention(place, lambdas, head_gain, came_q, key_blocks, half)
    returned = swap(sent_out, "ep", partner)
    kept_out = attention(place, lambdas, head_gain, q_keep, key_blocks, half)
    both = jnp.concatenate([kept_out, returned], axis=1)
    moved = [both[b * parts : (b + 1) * parts] for b in range(tp)]
    moved = [swap(block, "tp", b) if b else block for b, block in enumerate(moved)]
    half_rows = out_weight.shape[0] // 2
    first_rows = gather_all(out_weight[:half_rows], "tp", bits_below(tp))
    last_rows = gather_all(out_weight[half_rows:], "tp", bits_below(tp))
    mixer_out = mixer(place, moved, [w for pair in zip(first_rows, last_rows) for w in pair])

    replies = {}
    for group in groups:
        block = jnp.concatenate([arrived[k] for k in group], axis=0)
        blocks = gather_all(block, "tp", bits_below(tp))
        partial = expert(blocks, expert_gate[0], expert_up[0], expert_down[0])
        summed = scatter_tp(partial[:-1], partial[-1])
        for index, k in enumerate(group):
            piece = summed[index * cap : (index + 1) * cap]
            replies[k] = swap(piece, "ep", k) if k else piece
    expert_out = combine(hops, ranks, route_logits.T, [replies[k] for k in range(ep)])
    return (mixer_out, expert_out)


def solution(mesh):
    placed = (
        P("ep", "tp"),
        P("ep", "tp"),
        P("ep", "tp"),
        P("tp"),
        P(),
        P("tp", None),
        P(("ep", "tp"), None),
        P(),
        P(("ep", "tp"), None),
        P(("ep", "tp"), None),
        P("ep", None, "tp"),
        P("ep", None, "tp"),
        P("ep", "tp", None),
    )
    return jax.shard_map(
        per_device,
        mesh=mesh,
        in_specs=placed,
        out_specs=(P(("ep", "tp"), None), P(("ep", "tp"), None)),
        check_vma=False,
    )
```

```python
import functools

import jax
import jax.numpy as jnp
from jax import lax
from jax.experimental import pallas as pl
from jax.experimental.pallas import tpu as pltpu
from jax.sharding import PartitionSpec as P


epsilon = 1e-06
init_lambda = 0.2
small_vmem = 6 * 1024 * 1024
expert_vmem = 10 * 1024 * 1024
attention_margin = 3 * 1024 * 1024


whole_vmem = pl.BlockSpec(memory_space=pltpu.VMEM)


def capacity(tokens, top_count, experts):
    return max(2, (top_count * tokens * 5 + 4 * experts - 1) // (4 * experts))


def swap(array, axis, mask):
    size = lax.axis_size(axis)
    return lax.ppermute(array, axis, [(i, i ^ mask) for i in range(size)])


def dispatch_kernel(cap, place_ref, x_ref, gain_ref, routes_ref, hops_ref, ranks_ref, *blocks):
    tokens, _ = x_ref.shape
    rows = x_ref[...].astype(jnp.float32)
    mean_square = jnp.mean(rows * rows, axis=-1, keepdims=True)
    normed = (rows * lax.rsqrt(mean_square + epsilon) * gain_ref[...]).astype(jnp.bfloat16)
    count = len(blocks)
    top = routes_ref.shape[0]
    hops_ref[...] = routes_ref[...] ^ place_ref[0]
    earlier = lax.broadcasted_iota(jnp.int32, (tokens, tokens), 0)
    later = lax.broadcasted_iota(jnp.int32, (tokens, tokens), 1)
    before = (earlier < later).astype(jnp.float32).astype(jnp.bfloat16)
    hop_ids = lax.broadcasted_iota(jnp.int32, (count, tokens), 0)
    base = jnp.zeros((count, 1), jnp.float32)
    ranks = []
    for j in range(top):
        chosen = (hops_ref[j : j + 1, :] == hop_ids).astype(jnp.float32)
        prefix = jnp.dot(chosen.astype(jnp.bfloat16), before, preferred_element_type=jnp.float32)
        rank = jnp.sum(chosen * (prefix + base), axis=0, keepdims=True)
        base = base + jnp.sum(chosen, axis=1, keepdims=True)
        ranks.append(rank.astype(jnp.int32))
        ranks_ref[j : j + 1, :] = ranks[-1]
    places = lax.broadcasted_iota(jnp.int32, (cap, tokens), 0)
    picks = []
    for k in range(count):
        picked = jnp.zeros((cap, tokens), jnp.float32)
        for j in range(top):
            hit = (hops_ref[j : j + 1, :] == k) & (ranks[j] == places)
            picked = picked + hit.astype(jnp.float32)
        picks.append(picked)
    picks = jnp.concatenate(picks, axis=0).astype(jnp.bfloat16)
    rows = jnp.dot(picks, normed, preferred_element_type=jnp.float32)
    for k, block in enumerate(blocks):
        block[...] = rows[k * cap : (k + 1) * cap].astype(jnp.bfloat16)


def dispatch(place, moe_input, moe_gain, routes, cap, count):
    tokens, width = moe_input.shape
    shapes = [jax.ShapeDtypeStruct(routes.shape, jnp.int32)] * 2
    shapes += [jax.ShapeDtypeStruct((cap, width), jnp.bfloat16)] * count
    out = pl.pallas_call(
        functools.partial(dispatch_kernel, cap),
        out_shape=shapes,
        in_specs=[pl.BlockSpec(memory_space=pltpu.SMEM)] + [whole_vmem] * 3,
        out_specs=[whole_vmem] * len(shapes),
        cost_estimate=pl.CostEstimate(flops=2 * cap * count * tokens * width, bytes_accessed=4 * tokens * width, transcendentals=0),
        compiler_params=pltpu.CompilerParams(vmem_limit_bytes=small_vmem),
        name="dispatch",
    )(place, moe_input, moe_gain.reshape(1, -1), routes)
    return out[0], out[1], list(out[2:])


def pack_kernel(count, place_ref, q_ref, k_ref, v_ref, kept_ref, given_ref, q_keep_ref):
    first = place_ref[2] == 0
    parts = q_ref.shape[0] // count
    k_half, v_half = k_ref.shape[1] // 2, v_ref.shape[1] // 2

    def halves(array):
        width = array.shape[1] // 2
        low, high = array[:, :width], array[:, width:]
        return jnp.where(first, low, high), jnp.where(first, high, low)

    kept_ref[:, :k_half], given_ref[:, :k_half] = halves(k_ref[...])
    kept_ref[:, k_half:], given_ref[:, k_half : k_half + v_half] = halves(v_ref[...])
    for b in range(count):
        source = pl.ds(pl.multiple_of((place_ref[1] ^ b) * parts, parts), parts)
        at = slice(b * parts, (b + 1) * parts)
        q_keep_ref[at, :], given_ref[at, k_half + v_half :] = halves(q_ref[source, :])


def pack(place, queries, keys, values, count):
    rows = queries.shape[0]
    q_half, k_half, v_half = queries.shape[1] // 2, keys.shape[1] // 2, values.shape[1] // 2
    widths = (k_half + v_half, k_half + v_half + q_half, q_half)
    return pl.pallas_call(
        functools.partial(pack_kernel, count),
        out_shape=[jax.ShapeDtypeStruct((rows, width), jnp.bfloat16) for width in widths],
        in_specs=[pl.BlockSpec(memory_space=pltpu.SMEM)] + [whole_vmem] * 3,
        out_specs=[whole_vmem] * 3,
        compiler_params=pltpu.CompilerParams(vmem_limit_bytes=small_vmem),
        cost_estimate=pl.CostEstimate(flops=rows, bytes_accessed=8 * rows * widths[1], transcendentals=0),
        name="pack",
    )(place, queries, keys, values)


def window_kernel(ranks_ref, gate_ref, up_ref, down_ref, out_ref):
    out_ref[...] = ranks_ref[...]


def window(ranks, *weights):
    return pl.pallas_call(
        window_kernel,
        out_shape=jax.ShapeDtypeStruct(ranks.shape, ranks.dtype),
        in_specs=[whole_vmem] * (1 + len(weights)),
        out_specs=whole_vmem,
        compiler_params=pltpu.CompilerParams(vmem_limit_bytes=small_vmem),
        cost_estimate=pl.CostEstimate(flops=1, bytes_accessed=4 * ranks.size, transcendentals=0),
        name="window",
    )(ranks, *weights)


def combine_kernel(hops_ref, ranks_ref, logits_ref, *refs):
    blocks, out_ref = refs[:-1], refs[-1]
    top, tokens = hops_ref.shape
    cap = blocks[0].shape[0]
    logits = logits_ref[...]
    peak = jnp.max(logits, axis=0, keepdims=True)
    raised = jnp.exp(logits - peak)
    gates = raised / jnp.sum(raised, axis=0, keepdims=True)
    places = lax.broadcasted_iota(jnp.int32, (cap, tokens), 0)
    parts = []
    for k in range(len(blocks)):
        weight = jnp.zeros((cap, tokens), jnp.float32)
        for j in range(top):
            hit = (hops_ref[j : j + 1, :] == k) & (ranks_ref[j : j + 1, :] == places)
            weight = weight + jnp.where(hit, gates[j : j + 1, :], 0.0)
        parts.append(weight)
    weights = jnp.concatenate(parts, axis=0)
    high = weights.astype(jnp.bfloat16)
    low = (weights - high.astype(jnp.float32)).astype(jnp.bfloat16)
    rows = jnp.concatenate([block[...] for block in blocks], axis=0)
    both = lax.dot_general(
        jnp.concatenate([high, low], axis=1),
        rows,
        (((0,), (0,)), ((), ())),
        preferred_element_type=jnp.float32,
    )
    out_ref[...] = (both[:tokens] + both[tokens:]).astype(jnp.bfloat16)


def combine(hops, ranks, logits, blocks):
    tokens, width = hops.shape[1], blocks[0].shape[1]
    return pl.pallas_call(
        combine_kernel,
        out_shape=jax.ShapeDtypeStruct((tokens, width), jnp.bfloat16),
        in_specs=[whole_vmem] * (3 + len(blocks)),
        out_specs=whole_vmem,
        cost_estimate=pl.CostEstimate(flops=4 * tokens * width * len(blocks) * blocks[0].shape[0], bytes_accessed=4 * tokens * width, transcendentals=0),
        compiler_params=pltpu.CompilerParams(vmem_limit_bytes=small_vmem),
        name="combine",
    )(hops, ranks, logits, *blocks)


def expert_kernel(count, *refs):
    inputs = refs[:count]
    gate_ref, up_ref, down_ref = refs[count : count + 3]
    outputs = refs[count + 3 : -1]
    hidden_ref = refs[-1]
    _, width = inputs[0].shape
    tile, wide = 128, min(512, width)
    order = list(range(0, count, 2)) + list(range(1, count, 2))

    def hidden_step(step, carry):
        at = pl.ds(pl.multiple_of(step * tile, tile), tile)
        x = jnp.concatenate([inputs[i][...] for i in order], axis=0)
        both = jnp.concatenate([gate_ref[:, at], up_ref[:, at]], axis=1)
        product = jnp.dot(x, both, preferred_element_type=jnp.float32)
        gate_part, up_part = product[:, :tile], product[:, tile:]
        hidden = gate_part / (1.0 + jnp.exp(-gate_part)) * up_part
        hidden_ref[:, at] = hidden.astype(jnp.bfloat16)
        return carry

    def down_step(step, carry):
        at = pl.ds(pl.multiple_of(step * wide, wide), wide)
        product = jnp.dot(hidden_ref[...], down_ref[:, at], preferred_element_type=jnp.float32)
        first = 0
        for ref in outputs:
            ref[:, at] = product[first : first + ref.shape[0]].astype(jnp.bfloat16)
            first += ref.shape[0]
        return carry

    lax.fori_loop(0, gate_ref.shape[1] // tile, hidden_step, 0, unroll=True)
    lax.fori_loop(0, width // wide, down_step, 0, unroll=True)


def expert(blocks, gate, up, down):
    count = len(blocks)
    rows, width = blocks[0].shape
    units = gate.shape[1]
    stay = count - count // 2
    shapes = [jax.ShapeDtypeStruct((rows, width), jnp.bfloat16)] * stay
    shapes += [jax.ShapeDtypeStruct((rows * (count // 2), width), jnp.bfloat16)]
    return pl.pallas_call(
        functools.partial(expert_kernel, count),
        out_shape=shapes,
        in_specs=[whole_vmem] * (count + 3),
        out_specs=[whole_vmem] * len(shapes),
        scratch_shapes=[pltpu.VMEM((count * rows, units), jnp.bfloat16)],
        compiler_params=pltpu.CompilerParams(vmem_limit_bytes=expert_vmem),
        cost_estimate=pl.CostEstimate(
            flops=6 * count * rows * width * units,
            bytes_accessed=6 * width * units + 4 * count * rows * width,
            transcendentals=count * rows * units,
        ),
    )(*blocks, gate, up, down)


def attention_kernel(heads, head_size, value_size, rows, count, place_ref, lam_ref, gain_ref, q_ref, *refs):
    blocks, out_ref = refs[:count], refs[count]
    value_ref, score_a, score_b, peak_a, peak_b = refs[count + 1 :]
    tiles = q_ref.shape[0] // rows
    keys = blocks[0].shape[0]
    pair = 2 * head_size
    scale = head_size ** (-0.5)
    lanes = lax.broadcasted_iota(jnp.int32, (rows, pair), 1)

    for head in range(heads):
        lam = lam_ref[place_ref[2] * heads + head]
        first_value = heads * pair + head * value_size

        for index, block in enumerate(blocks):
            at = slice(index * keys, (index + 1) * keys)
            value_ref[at, :value_size] = block[:, first_value : first_value + value_size]
            value_ref[at, value_size:] = jnp.ones((keys, value_size), jnp.bfloat16)

        def step(following, score_to, peak_to, current, score_from, peak_from):
            if following is not None:
                at = pl.ds(pl.multiple_of(following * rows, rows), rows)
                q = q_ref[at, head * pair : (head + 1) * pair].astype(jnp.float32) * scale
                q = jnp.concatenate(
                    [jnp.where(lanes < head_size, q, 0.0), jnp.where(lanes < head_size, 0.0, q)], axis=0
                ).astype(jnp.bfloat16)
                peak = jnp.full((2 * rows, 128), -jnp.inf, jnp.float32)
            if current is not None:
                maxima = jnp.concatenate([peak_from[...]] * (keys // 128), axis=1)
                total = jnp.zeros((2 * rows, 2 * value_size), jnp.float32)
            for index, block in enumerate(blocks):
                columns = slice(index * keys, (index + 1) * keys)
                if following is not None:
                    scores = lax.dot_general(
                        q,
                        block[:, head * pair : (head + 1) * pair],
                        (((1,), (1,)), ((), ())),
                        preferred_element_type=jnp.float32,
                    )
                    score_to[:, columns] = scores
                    for part in range(keys // 128):
                        peak = jnp.maximum(peak, scores[:, part * 128 : (part + 1) * 128])
                if current is not None:
                    weights = jnp.exp(score_from[:, columns] - maxima)
                    total = total + jnp.dot(
                        weights.astype(jnp.bfloat16),
                        value_ref[columns, :],
                        preferred_element_type=jnp.float32,
                    )
            if following is not None:
                peak_to[...] = jnp.broadcast_to(jnp.max(peak, axis=1, keepdims=True), peak.shape)
            if current is not None:
                maps = total[:, :value_size] / total[:, value_size:]
                head_out = maps[:rows] - lam * maps[rows:]
                mean_square = jnp.mean(head_out * head_out, axis=-1, keepdims=True)
                normal = head_out * lax.rsqrt(mean_square + epsilon) * gain_ref[...] * (1.0 - init_lambda)
                out_at = pl.ds(pl.multiple_of(current * rows, rows), rows)
                out_ref[out_at, head * value_size : (head + 1) * value_size] = normal.astype(jnp.bfloat16)

        def two_tiles(i, carry):
            step(2 * i + 1, score_b, peak_b, 2 * i, score_a, peak_a)
            step(2 * i + 2, score_a, peak_a, 2 * i + 1, score_b, peak_b)
            return carry

        step(0, score_a, peak_a, None, None, None)
        if tiles > 2:
            lax.fori_loop(0, tiles // 2 - 1, two_tiles, 0)
        step(tiles - 1, score_b, peak_b, tiles - 2, score_a, peak_a)
        step(None, None, None, tiles - 1, score_b, peak_b)


def attention(place, lam, gain, q, blocks, heads):
    value_size = gain.shape[0]
    head_size = q.shape[1] // (2 * heads)
    queries = q.shape[0]
    keys = blocks[0].shape[0]
    total_keys = keys * len(blocks)
    rows = min(256, queries // 2)
    while rows > 16 and 8 * rows * total_keys > 2**23:
        rows //= 2
    smem = pl.BlockSpec(memory_space=pltpu.SMEM)
    scratch = 4 * total_keys * value_size + 16 * rows * (total_keys + 128)
    room = scratch + 2 * blocks[0].size * len(blocks) + attention_margin
    scratch = 4 * total_keys * value_size + 16 * rows * (total_keys + 128)
    room = scratch + 2 * blocks[0].size * len(blocks) + attention_margin
    return pl.pallas_call(
        functools.partial(attention_kernel, heads, head_size, value_size, rows, len(blocks)),
        out_shape=jax.ShapeDtypeStruct((queries, heads * value_size), jnp.bfloat16),
        in_specs=[smem, smem] + [whole_vmem] * (2 + len(blocks)),
        out_specs=whole_vmem,
        scratch_shapes=[pltpu.VMEM((total_keys, 2 * value_size), jnp.bfloat16)]
        + [pltpu.VMEM((2 * rows, total_keys), jnp.float32)] * 2
        + [pltpu.VMEM((2 * rows, 128), jnp.float32)] * 2,
        compiler_params=pltpu.CompilerParams(vmem_limit_bytes=room),
        cost_estimate=pl.CostEstimate(
            flops=heads * queries * total_keys * 2 * 2 * (head_size + value_size) * 2,
            bytes_accessed=2 * total_keys * heads * (2 * head_size + value_size),
            transcendentals=2 * heads * queries * total_keys,
        ),
    )(place, lam, gain.reshape(1, -1), q, *blocks)


def mixer_kernel(count, place_ref, *refs):
    columns, weights, out_ref = refs[:count], refs[count:-1], refs[-1]
    half = columns[0].shape[1] // 2
    first = place_ref[2] == 0
    ordered = []
    for ref in columns:
        kept, other = ref[:, :half], ref[:, half:]
        ordered += [jnp.where(first, kept, other), jnp.where(first, other, kept)]
    out_ref[...] = jnp.dot(
        jnp.concatenate(ordered, axis=1),
        jnp.concatenate([ref[...] for ref in weights], axis=0),
        preferred_element_type=jnp.float32,
    ).astype(jnp.bfloat16)


def mixer(place, columns, weights):
    rows, width = columns[0].shape[0], weights[0].shape[1]
    return pl.pallas_call(
        functools.partial(mixer_kernel, len(columns)),
        out_shape=jax.ShapeDtypeStruct((rows, width), jnp.bfloat16),
        in_specs=[pl.BlockSpec(memory_space=pltpu.SMEM)] + [whole_vmem] * (len(columns) + len(weights)),
        out_specs=whole_vmem,
        compiler_params=pltpu.CompilerParams(vmem_limit_bytes=expert_vmem),
        cost_estimate=pl.CostEstimate(
            flops=2 * rows * width * sum(w.shape[0] for w in weights),
            bytes_accessed=2 * width * sum(w.shape[0] for w in weights),
            transcendentals=0,
        ),
        name="mixer",
    )(place, *columns, *weights)


def gather_all(block, axis, bits):
    held = {0: block}
    for bit in bits:
        for index in list(held):
            held[index ^ bit] = swap(held[index], axis, bit)
    return [held[i] for i in sorted(held)]


def bits_below(size):
    bits = []
    while size > 1:
        size //= 2
        bits.append(size)
    return bits


def key_bits(ep):
    return bits_below(ep)[:1] + bits_below(ep)[2:]


def scatter_tp(stay, sent):
    came = swap(sent, "tp", 1)
    rows = stay[0].shape[0]
    held = {}
    for i in reversed(range(len(stay))):
        held[2 * i] = add_rounded(stay[i], came[i * rows : (i + 1) * rows])
    bit = 2
    while bit < 2 * len(stay):
        for index in [i for i in sorted(held, reverse=True) if i & bit]:
            came = swap(held.pop(index), "tp", bit)
            held[index ^ bit] = add_rounded(held[index ^ bit], came)
        bit *= 2
    return held[0]


def add_rounded(first, second):
    return (first.astype(jnp.float32) + second.astype(jnp.float32)).astype(jnp.bfloat16)


def per_device(
    queries,
    key_rows,
    value_rows,
    lambdas,
    head_gain,
    out_weight,
    moe_input,
    moe_gain,
    routes,
    route_logits,
    expert_gate,
    expert_up,
    expert_down,
):
    ep, tp = lax.axis_size("ep"), lax.axis_size("tp")
    me, column = lax.axis_index("ep"), lax.axis_index("tp")
    far = ep // 2
    tokens, top_count = routes.shape
    cap = capacity(tokens, top_count, ep)

    partner = far // 2
    place = jnp.stack([me, column, (me // partner) % 2]).astype(jnp.int32)
    hops, ranks, outgoing = dispatch(place, moe_input, moe_gain, routes.T, cap, ep)
    ranks = window(ranks, expert_gate[0], expert_up[0], expert_down[0])
    quarter = ep // 4
    groups = [range(0, far), range(far, far + quarter), range(far + quarter, ep)]

    local_rows, local_heads = queries.shape[0], lambdas.shape[0]
    half = local_heads // 2
    kept, given, q_keep = pack(place, queries, key_rows, value_rows, tp)
    came = swap(given, "ep", partner)
    kv_width = kept.shape[1]
    parts = local_rows // tp
    came_kv, came_q = came[:, :kv_width], came[:, kv_width:]
    key_blocks = gather_all(kept, "ep", key_bits(ep)) + gather_all(came_kv, "ep", key_bits(ep))

    arrived = {0: outgoing[0]}
    for group in (groups[1], groups[0], groups[2]):
        for k in group:
            if k:
                arrived[k] = swap(outgoing[k], "ep", k)

    sent_out = attention(place, lambdas, head_gain, came_q, key_blocks, half)
    returned = swap(sent_out, "ep", partner)
    kept_out = attention(place, lambdas, head_gain, q_keep, key_blocks, half)
    both = jnp.concatenate([kept_out, returned], axis=1)
    moved = [both[b * parts : (b + 1) * parts] for b in range(tp)]
    moved = [swap(block, "tp", b) if b else block for b, block in enumerate(moved)]
    half_rows = out_weight.shape[0] // 2
    first_rows = gather_all(out_weight[:half_rows], "tp", bits_below(tp))
    last_rows = gather_all(out_weight[half_rows:], "tp", bits_below(tp))
    mixer_out = mixer(place, moved, [w for pair in zip(first_rows, last_rows) for w in pair])

    replies = {}
    for group in groups:
        block = jnp.concatenate([arrived[k] for k in group], axis=0)
        blocks = gather_all(block, "tp", bits_below(tp))
        partial = expert(blocks, expert_gate[0], expert_up[0], expert_down[0])
        summed = scatter_tp(partial[:-1], partial[-1])
        for index, k in enumerate(group):
            piece = summed[index * cap : (index + 1) * cap]
            replies[k] = swap(piece, "ep", k) if k else piece
    expert_out = combine(hops, ranks, route_logits.T, [replies[k] for k in range(ep)])
    return (mixer_out, expert_out)


def solution(mesh):
    placed = (
        P("ep", "tp"),
        P("ep", "tp"),
        P("ep", "tp"),
        P("tp"),
        P(),
        P("tp", None),
        P(("ep", "tp"), None),
        P(),
        P(("ep", "tp"), None),
        P(("ep", "tp"), None),
        P("ep", None, "tp"),
        P("ep", None, "tp"),
        P("ep", "tp", None),
    )
    return jax.shard_map(
        per_device,
        mesh=mesh,
        in_specs=placed,
        out_specs=(P(("ep", "tp"), None), P(("ep", "tp"), None)),
        check_vma=False,
    )
```
